32 devices in a mesh: sp: 8 (over z, y), tp: 4 (over x, core).
Axes of the slice: x: 2, y: 2, z: 4, core: 2. Of those that a mesh axis runs over, the one named last changes fastest.
Arguments:
- resid: bfloat16 [2048, 2048], P(('sp', 'tp')), may hold values from -6 to 6
- queries: bfloat16 [2048, 1024], P('sp', 'tp'), may hold values from -6 to 6
- keys: bfloat16 [2048, 256], P('sp', 'tp'), may hold values from -6 to 6
- values: bfloat16 [2048, 256], P('sp', 'tp'), may hold values from -6 to 6
- docs: int32 [2048], P('sp'), may hold values from 0 to 3, never falling along the last dimension, each value on 1 to 1024 neighbouring positions
- q_gain: float32 [64], replicated, may hold values from 0.1 to 1.9
- key_norm_gain: float32 [64], replicated, may hold values from 0.1 to 1.9
- sink: float32 [16], P('tp'), may hold values from 4 to 8
- out_gain: float32 [1024], replicated, may hold values from 0.1 to 1.9
- w_out: bfloat16 [1024, 2048], replicated, may hold values from -0.1875 to 0.1875
- norm_gain: float32 [2048], replicated, may hold values from 0.1 to 1.9
- routes: int32 [2048, 4], P('sp'), may hold values from 0 to 7, all different within a row; in each aligned block of 64 rows (0 to 63, 64 to 127, ...) at most 50 rows name the same one
- route_weights: float32 [2048, 4], P(('sp', 'tp')), may hold values from 0.1 to 1
- w_gate: bfloat16 [8, 2048, 2048], P('sp', None, 'tp'), may hold values from -0.375 to 0.375
- w_up: bfloat16 [8, 2048, 2048], P('sp', None, 'tp'), may hold values from -0.375 to 0.375
- w_down: bfloat16 [8, 2048, 2048], P('sp', 'tp'), may hold values from -0.015625 to 0.015625
Outputs:
- layer_out: bfloat16 [2048, 2048], P(('sp', 'tp'))
The draws below stay inside these ranges and needn't reach their ends.
Inputs may be any that keep to these rules, and one draw needn't show every extreme that they name: `routes`: in each aligned block of 64 tokens no expert is named more than 50 times, and some expert is named exactly that often; the 4 experts of a token differ. `docs`: document numbers never fall along the sequence, and each document has 1 to 1024 positions.
All inputs are finite; a program needn't handle non-finite values.
Results may differ from the reference program's by a relative error of at most 0.015.
Values may be sent and summed in bfloat16 or wider, within the bound.
A program may use at most 128 MiB of HBM per device.

```python
import math
import jax
import jax.numpy as jnp
import numpy as np
from jax import lax

D = 2048
QUERY_HEAD_COUNT = 16
KEY_VALUE_HEADS = 4
HEAD_DIMENSION = 64
ATT = 1024
FF = 2048
EXPERTS = 8
TOP = 4
WINDOW = 128
TOK_DEV = 256
PACKED_TOKENS = 2048
TQ = 64
CAP_SLOT = 50
DOCS = 4
DOC_SPAN = 1024
N_SP = 8
N_TP = 4


def block_levels(own_key, shape, shards, least, largest):
    def one(dim, blocks):
        steps = jax.random.uniform(jax.random.fold_in(jax.random.fold_in(own_key, 6), dim), (blocks,), jnp.float32, least / len(shards), largest / len(shards))
        return jnp.repeat(jnp.exp(steps), shape[dim] // blocks).reshape((-1,) + (1,) * (len(shape) - dim - 1))

    gain = one(*shards[0])
    for cut in shards[1:]:
        gain = gain * one(*cut)
    return gain


def split_up(count, total, reach, skew):
    weights = [(1 << 20) // math.isqrt(rank ** skew) + 1 for rank in range(2, count + 1)]
    spare, counts = total - reach - (count - 1), [1] * (count - 1)
    while spare > 0:
        candidates = [i for i in range(count - 1) if counts[i] < reach]
        pool, left = sum([weights[i] for i in candidates]), spare
        for i in candidates:
            addition = min(reach - counts[i], max(1, left * weights[i] // pool), spare)
            counts[i] = counts[i] + addition
            spare = spare - addition
    return np.array([reach] + counts)


def uneven_parts(key, number_of, total, reach, skew):
    if number_of == 2:
        one = jax.random.randint(key, (), max(1, total - reach), min(reach, total - 1) + 1)
        return jnp.stack([one, total - one])
    lengths = jnp.asarray(split_up(number_of, total, reach, skew), jnp.int32)
    twos = (number_of - 1) // 2
    giver, taker = lengths[1:1 + 2 * twos:2], lengths[2:2 + 2 * twos:2]
    margin = jnp.minimum(giver - 1, reach - taker)
    shifted = jax.random.randint(jax.random.fold_in(key, 1), (twos,), 0, 1 << 20) % (margin + 1)
    lengths = lengths.at[1:1 + 2 * twos:2].set(giver - shifted).at[2:2 + 2 * twos:2].set(taker + shifted)
    return lengths[jax.random.permutation(jax.random.fold_in(key, 2), number_of)]


def routed_block(own_key, own, number, rows, number_of, top, most, slope):
    ranking = jax.random.permutation(own_key, number_of)
    crowded, common = load_shares(number_of, rows * top, most, slope, True), load_shares(number_of, rows * top, most, slope, False)
    places = jnp.arange(number_of)

    def named(lengths, offset_by):
        used = int((lengths > 0).sum())
        fixed = max(1, used // 4)
        passed = fixed + (places - fixed + offset_by * (used - fixed)) % max(1, number_of - fixed)
        return jnp.zeros((number_of,), jnp.int32).at[ranking[jnp.where(places < fixed, places, passed)]].set(jnp.asarray(lengths, jnp.int32))

    lengths = jnp.where(number % 4 == 0, named(crowded, number // 4), named(common, number - number // 4 - 1))
    mixed = jax.random.permutation(jax.random.fold_in(own, 3), number_of)
    donor, taker = mixed[0:number_of // 2 * 2:2], mixed[1:number_of // 2 * 2:2]
    room = jnp.minimum(lengths[donor] - 1, most - lengths[taker]) // 2
    room = jnp.where((donor == ranking[0]) | (taker == ranking[0]) | (lengths[taker] == 0), 0, jnp.maximum(room, 0))
    passed = jax.random.randint(jax.random.fold_in(own, 4), (number_of // 2,), 0, 1 << 20) % (room + 1)
    lengths = lengths.at[donor].add(-passed).at[taker].add(passed)
    items = jnp.searchsorted(jnp.cumsum(lengths), jnp.arange(rows * top), side="right").astype(jnp.int32)
    grid = items.reshape(top, rows).T
    grid = grid[jax.random.permutation(jax.random.fold_in(own, 1), rows)]
    offset_by = jax.random.randint(jax.random.fold_in(own, 2), (rows, 1), 0, top)
    return jnp.take_along_axis(grid, (jnp.arange(top)[None, :] + offset_by) % top, axis=1)


def load_shares(count, total, limit, lean, full):
    loads = [(1 << 20) // math.isqrt(rank ** lean) + 1 for rank in range(1, count + 1)]
    largest = limit if full else min(limit, max(-(-total // count), total * loads[0] // sum(loads)))
    least = 1 if total - largest >= count - 1 else 0
    counts, rest = [largest] + [least] * (count - 1), total - largest - least * (count - 1)
    while rest > 0:
        candidates = [i for i in range(1, count) if counts[i] < largest] or [i for i in range(1, count) if counts[i] < limit]
        mass, remaining = sum([loads[i] for i in candidates]), rest
        for i in candidates:
            addition = min(limit - counts[i], max(1, remaining * loads[i] // mass), rest)
            counts[i] = counts[i] + addition
            rest = rest - addition
    return np.array(counts)


def gaussian(rng, shape, spread, bound, shards=(), kind=jnp.bfloat16):
    level = block_levels(rng, shape, shards, -0.22, 0.18) if shards else 1.0
    array = jax.random.normal(rng, shape, jnp.float32) * spread * level
    return jnp.minimum(jnp.maximum(array, -bound), bound).astype(kind)


def setup_inputs(seed: int = 0) -> dict:
    arg_keys = jax.random.split(jax.random.key(seed), 17)
    resid = gaussian(arg_keys[0], (PACKED_TOKENS, D), 1.0, 6.0, ((0, 32),))
    queries = gaussian(arg_keys[1], (PACKED_TOKENS, ATT), 1.0, 6.0, ((0, 8), (1, 4)))
    keys = gaussian(arg_keys[2], (PACKED_TOKENS, KEY_VALUE_HEADS * HEAD_DIMENSION), 1.0, 6.0, ((0, 8), (1, 4)))
    values = gaussian(arg_keys[3], (PACKED_TOKENS, KEY_VALUE_HEADS * HEAD_DIMENSION), 1.0, 6.0, ((0, 8), (1, 4)))
    docs = jnp.searchsorted(jnp.cumsum(uneven_parts(arg_keys[4], DOCS, PACKED_TOKENS, DOC_SPAN, 2)), jnp.arange(PACKED_TOKENS), side="right").astype(jnp.int32)
    q_gain = jnp.clip(1.0 + 0.18 * jax.random.normal(arg_keys[5], (HEAD_DIMENSION,), jnp.float32), 0.1, 1.9)
    key_norm_gain = jnp.clip(1.0 + 0.18 * jax.random.normal(arg_keys[6], (HEAD_DIMENSION,), jnp.float32), 0.1, 1.9)
    sink = jnp.clip(4.0 + 4.0 * jax.random.uniform(arg_keys[7], (QUERY_HEAD_COUNT,), jnp.float32) ** block_levels(arg_keys[7], (QUERY_HEAD_COUNT,), ((0, 4),), -0.2, 0.2), 4.0, 8.0)
    out_gain = jnp.clip(1.0 + 0.18 * jax.random.normal(arg_keys[8], (ATT,), jnp.float32), 0.1, 1.9)
    w_out = gaussian(arg_keys[9], (ATT, D), ATT ** -0.5, 0.1875)
    norm_gain = jnp.clip(1.0 + 0.18 * jax.random.normal(arg_keys[10], (D,), jnp.float32), 0.1, 1.9)
    routes_keys = jax.random.split(jax.random.fold_in(arg_keys[11], 1), PACKED_TOKENS // TQ)
    routes_turns = jax.random.permutation(jax.random.fold_in(arg_keys[11], 3), PACKED_TOKENS // TQ)
    routes = jax.vmap(lambda own, number: routed_block(jax.random.fold_in(arg_keys[11], 2), own, number, TQ, EXPERTS, TOP, CAP_SLOT, 2))(routes_keys, routes_turns).reshape((PACKED_TOKENS, TOP))
    route_weights = jnp.clip(0.1 + 0.9 * jax.random.uniform(arg_keys[12], (PACKED_TOKENS, TOP), jnp.float32) ** block_levels(arg_keys[12], (PACKED_TOKENS, TOP), ((0, 32),), -0.2, 0.2), 0.1, 1.0)
    w_gate = gaussian(arg_keys[13], (EXPERTS, D, FF), (D // 9) ** -0.5, 0.375, ((0, 8), (2, 4)))
    w_up = gaussian(arg_keys[14], (EXPERTS, D, FF), (D // 9) ** -0.5, 0.375, ((0, 8), (2, 4)))
    w_down = gaussian(arg_keys[15], (EXPERTS, FF, D), (64 * FF) ** -0.5, 0.015625, ((0, 8), (1, 4)))
    return dict(resid=resid, queries=queries, keys=keys, values=values, docs=docs, q_gain=q_gain, key_norm_gain=key_norm_gain, sink=sink, out_gain=out_gain, w_out=w_out, norm_gain=norm_gain, routes=routes, route_weights=route_weights, w_gate=w_gate, w_up=w_up, w_down=w_down)


rope_base = 10000.0
norm_eps = 1e-06
swiglu_limit = 7.0
swiglu_alpha = 1.702

def row_normalize(values, gain_vec):
    floats = values.astype(jnp.float32)
    scale_inv = lax.rsqrt(lax.optimization_barrier(jnp.mean(floats * floats, axis=-1, keepdims=True)) + norm_eps)
    return floats * scale_inv * gain_vec.astype(jnp.float32)

def apply_rotary_heads(heads, token_positions):
    half_size = heads.shape[-1] // 2
    freqs = rope_base ** (-jnp.arange(half_size, dtype=jnp.float32) / half_size)
    angles = token_positions[:, None] * freqs[None, :]
    cosine = jnp.cos(angles)[:, None, :]
    sine = jnp.sin(angles)[:, None, :]
    first_half = heads[..., :half_size]
    second_half = heads[..., half_size:]
    return jnp.concatenate([first_half * cosine - second_half * sine, first_half * sine + second_half * cosine], axis=-1)

def expert_act(gate_pre, up_pre):
    gate_cut = jnp.minimum(gate_pre, swiglu_limit)
    up_cut = jnp.clip(up_pre, -swiglu_limit, swiglu_limit)
    return (up_cut + 1.0) * gate_cut * jax.nn.sigmoid(swiglu_alpha * gate_cut)

def slot_tables(route_block, expert_count, capacity):
    pair_total = route_block.shape[1]
    expert_ids = jnp.arange(expert_count, dtype=jnp.int32)
    onehot = (route_block[:, :, None] == expert_ids[None, None, :]).astype(jnp.int32)
    before = jnp.cumsum(onehot, axis=1).astype(jnp.int32) - onehot
    rank = lax.optimization_barrier(jnp.sum(before * onehot, axis=-1)).astype(jnp.int32)
    pair_slot = (route_block * capacity + rank).astype(jnp.int32)
    slot_ids = jnp.arange(expert_count * capacity, dtype=jnp.int32)
    match = pair_slot[:, :, None] == slot_ids[None, None, :]
    pair_ids = jnp.arange(pair_total, dtype=jnp.int32)
    slot_pair = lax.optimization_barrier(jnp.sum(jnp.where(match, pair_ids[None, :, None], 0), axis=1)).astype(jnp.int32)
    filled = jnp.any(match, axis=1)
    return (pair_slot, slot_pair, filled)

def reference(resid, queries, keys, values, docs, q_gain, key_norm_gain, sink, out_gain, w_out, norm_gain, routes, route_weights, w_gate, w_up, w_down):
    query_group_width = QUERY_HEAD_COUNT // KEY_VALUE_HEADS
    token_positions = jnp.arange(PACKED_TOKENS, dtype=jnp.float32)
    q_rot = apply_rotary_heads(row_normalize(queries.reshape(PACKED_TOKENS, QUERY_HEAD_COUNT, HEAD_DIMENSION), q_gain), token_positions).astype(jnp.bfloat16)
    key_rotated = apply_rotary_heads(row_normalize(keys.reshape(PACKED_TOKENS, KEY_VALUE_HEADS, HEAD_DIMENSION), key_norm_gain), token_positions).astype(jnp.bfloat16)
    value_head_rows = values.reshape(PACKED_TOKENS, KEY_VALUE_HEADS, HEAD_DIMENSION)
    k_pad = jnp.pad(key_rotated, ((WINDOW, WINDOW), (0, 0), (0, 0)))
    v_pad = jnp.pad(value_head_rows, ((WINDOW, WINDOW), (0, 0), (0, 0)))
    doc_pad = jnp.pad(docs, (WINDOW, WINDOW), constant_values=-1)
    block_row_list = math.gcd(512, PACKED_TOKENS)
    span_rows = block_row_list + 2 * WINDOW
    scale = HEAD_DIMENSION ** (-0.5)
    sink_exponent = jnp.exp(sink.astype(jnp.float32)).reshape(KEY_VALUE_HEADS, query_group_width)

    def attend(block_id):
        first_row = (block_id * block_row_list).astype(jnp.int32)
        query_block_tile = lax.dynamic_slice_in_dim(q_rot, first_row, block_row_list, 0)
        query_block_tile = query_block_tile.reshape(block_row_list, KEY_VALUE_HEADS, query_group_width, HEAD_DIMENSION).astype(jnp.float32)
        k_block = lax.dynamic_slice_in_dim(k_pad, first_row, span_rows, 0).astype(jnp.float32)
        v_block = lax.dynamic_slice_in_dim(v_pad, first_row, span_rows, 0).astype(jnp.float32)
        doc_query = lax.dynamic_slice_in_dim(docs, first_row, block_row_list, 0)
        doc_key = lax.dynamic_slice_in_dim(doc_pad, first_row, span_rows, 0)
        scores = jnp.einsum('qhgd,khd->hgqk', query_block_tile, k_block) * scale
        offsets = jnp.arange(block_row_list, dtype=jnp.int32)[:, None] - (jnp.arange(span_rows, dtype=jnp.int32)[None, :] - WINDOW)
        allowed = (jnp.abs(offsets) <= WINDOW) & (doc_query[:, None] == doc_key[None, :])
        raw_weights = jnp.where(allowed[None, None], jnp.exp(scores), jnp.zeros((), jnp.float32))
        total = lax.optimization_barrier(jnp.sum(raw_weights, axis=-1)) + sink_exponent[:, :, None]
        probs = (raw_weights / total[..., None]).astype(jnp.bfloat16)
        mixed = jnp.einsum('hgqk,khd->qhgd', probs.astype(jnp.float32), v_block)
        return mixed.reshape(block_row_list, QUERY_HEAD_COUNT * HEAD_DIMENSION).astype(jnp.bfloat16)
    att = lax.map(attend, jnp.arange(PACKED_TOKENS // block_row_list, dtype=jnp.int32)).reshape(PACKED_TOKENS, QUERY_HEAD_COUNT * HEAD_DIMENSION)
    att_normed = row_normalize(att, out_gain).astype(jnp.bfloat16)
    middle = (resid.astype(jnp.float32) + jnp.dot(att_normed, w_out, preferred_element_type=jnp.float32)).astype(jnp.bfloat16)
    moe_in = row_normalize(middle, norm_gain).astype(jnp.bfloat16)
    quarter = TOK_DEV // N_TP
    block_count = N_SP * N_TP
    pair_total = quarter * TOP
    pair_slot, slot_pair, filled = slot_tables(routes.reshape(block_count, pair_total), EXPERTS, CAP_SLOT)
    slot_pair = slot_pair.reshape(block_count, EXPERTS, CAP_SLOT).transpose(1, 0, 2)
    filled = filled.reshape(block_count, EXPERTS, CAP_SLOT).transpose(1, 0, 2)
    block_base = (jnp.arange(block_count, dtype=jnp.int32) * quarter)[:, None]
    hidden_group = FF // N_TP

    def one_expert(accum, inputs):
        pair_ids, used, gate_w, up_w, down_w = inputs
        token_ids = (block_base + pair_ids // TOP).reshape(-1).astype(jnp.int32)
        route_slot = (pair_ids % TOP).reshape(-1).astype(jnp.int32)
        rows_in = moe_in[token_ids]
        gate_pre = jnp.dot(rows_in, gate_w, preferred_element_type=jnp.float32)
        up_pre = jnp.dot(rows_in, up_w, preferred_element_type=jnp.float32)
        hidden = expert_act(gate_pre, up_pre).astype(jnp.bfloat16)
        summed = jnp.zeros((rows_in.shape[0], D), jnp.float32)
        for group_id in range(N_TP):
            part = jnp.dot(hidden[:, group_id * hidden_group:(group_id + 1) * hidden_group], down_w[group_id * hidden_group:(group_id + 1) * hidden_group], preferred_element_type=jnp.float32)
            summed = summed + lax.optimization_barrier(part.astype(jnp.bfloat16)).astype(jnp.float32)
        expert_out = lax.optimization_barrier(summed.astype(jnp.bfloat16)).astype(jnp.float32)
        weight = route_weights[token_ids, route_slot] * used.reshape(-1).astype(jnp.float32)
        accum = accum.at[token_ids].add(weight[:, None] * expert_out)
        return (accum, None)
    accum, unused = lax.scan(one_expert, jnp.zeros((PACKED_TOKENS, D), jnp.float32), (slot_pair, filled, w_gate, w_up, w_down))
    return (middle.astype(jnp.float32) + accum).astype(jnp.bfloat16)
```

```python
import functools

import jax
import jax.numpy as jnp
from jax import lax
from jax.experimental import pallas as pl
from jax.experimental.pallas import tpu as pltpu
from jax.sharding import PartitionSpec as P

WINDOW = 128


rope_base = 10000.0
norm_eps = 1e-06
swiglu_limit = 7.0
swiglu_alpha = 1.702


def row_normalize(values, gain_vec):
    floats = values.astype(jnp.float32)
    scale_inv = lax.rsqrt(jnp.mean(floats * floats, axis=-1, keepdims=True) + norm_eps)
    return floats * scale_inv * gain_vec


def apply_rotary_heads(heads, token_positions):
    half_size = heads.shape[-1] // 2
    freqs = rope_base ** (-jnp.arange(half_size, dtype=jnp.float32) / half_size)
    angles = token_positions[:, None] * freqs[None, :]
    cosine = jnp.cos(angles)[:, None, :]
    sine = jnp.sin(angles)[:, None, :]
    first_half = heads[..., :half_size]
    second_half = heads[..., half_size:]
    return jnp.concatenate(
        [first_half * cosine - second_half * sine, first_half * sine + second_half * cosine],
        axis=-1,
    )


def expert_act(gate_pre, up_pre):
    gate_cut = jnp.minimum(gate_pre, swiglu_limit)
    up_cut = jnp.clip(up_pre, -swiglu_limit, swiglu_limit)
    return (up_cut + 1.0) * gate_cut * jax.nn.sigmoid(swiglu_alpha * gate_cut)


def slot_tables(route_block, expert_count, capacity):
    pair_total = route_block.shape[1]
    expert_ids = jnp.arange(expert_count, dtype=jnp.int32)
    onehot = (route_block[:, :, None] == expert_ids[None, None, :]).astype(jnp.int32)
    before = jnp.cumsum(onehot, axis=1) - onehot
    rank = jnp.sum(before * onehot, axis=-1)
    pair_slot = route_block * capacity + rank
    slot_ids = jnp.arange(expert_count * capacity, dtype=jnp.int32)
    match = pair_slot[:, :, None] == slot_ids[None, None, :]
    pair_ids = jnp.arange(pair_total, dtype=jnp.int32)
    slot_pair = jnp.sum(jnp.where(match, pair_ids[None, :, None], 0), axis=1)
    filled = jnp.any(match, axis=1)
    return (pair_slot, slot_pair, filled)


def expert_partial(arrived_rows, w_gate, w_up, w_down):
    lead_shape = arrived_rows.shape
    local_experts = w_gate.shape[0]
    grouped = arrived_rows.reshape(-1, local_experts, lead_shape[2] // local_experts, lead_shape[3])
    gate_pre = jnp.einsum("recd,edf->recf", grouped, w_gate, preferred_element_type=jnp.float32)
    up_pre = jnp.einsum("recd,edf->recf", grouped, w_up, preferred_element_type=jnp.float32)
    hidden = expert_act(gate_pre, up_pre).astype(jnp.bfloat16)
    partial_value = jnp.einsum("recf,efd->recd", hidden, w_down, preferred_element_type=jnp.float32)
    return (
        lax.optimization_barrier(partial_value.astype(jnp.bfloat16))
        .astype(jnp.float32)
        .reshape(lead_shape)
    )


LANES = 128
VMEM_LIMIT = 60 * 1024 * 1024
MESH = pl.DeviceIdType.MESH


def moe_kernel(
    zn, x_in, mid, wg_hbm, wu_hbm, wd_hbm, out,
    X, S, P1, crecv, rx, ry, rdx, rdy, zbuf, acc, wg, wu, wd,
    wsem, az_s, az_r, ag_s, ag_r, c_s, c_r, rs_s, rs_r, rz_s, rz_r,
):
    sp, tp = lax.axis_index("sp"), lax.axis_index("tp")
    z, y = sp // 2, sp % 2
    xx, c = tp // 2, tp % 2
    T, W = x_in.shape
    D = out.shape[1]
    H = D // 2
    F = wg.shape[1]
    ynb = (z * 2 + (1 - y), tp)
    xnb = (sp, (1 - xx) * 2 + c)
    cnb = (sp, xx * 2 + (1 - c))

    def plane(zz):
        return (zz * 2 + y, tp)

    turn = 2 * (2 * z // zn) - 1
    far_first = [(z + turn * (1 + k) + 2 * zn) % zn for k in range(zn - 1)] + [z]

    loads = [
        pltpu.make_async_copy(src.at[0], dst, wsem.at[i])
        for i, (src, dst) in enumerate(((wg_hbm, wg), (wu_hbm, wu), (wd_hbm, wd)))
    ]
    for load in loads:
        load.start()

    bar = pltpu.get_barrier_semaphore()
    for nb in (ynb, xnb, cnb, *(plane(zz) for zz in far_first[:-1])):
        pl.semaphore_signal(bar, inc=1, device_id=nb, device_id_type=MESH)
    pl.semaphore_wait(bar, 3 + zn - 1)

    def rows(zz):
        return pl.ds(pl.multiple_of(zz * T, T), T)

    def rc(src, dst, ss, rs, dev):
        return pltpu.make_async_remote_copy(
            src_ref=src, dst_ref=dst, send_sem=ss, recv_sem=rs, device_id=dev, device_id_type=MESH
        )

    A, B = pl.ds(0, H), pl.ds(H, W - H)

    def ag(kind, zz, own=False):
        table = {
            "y": (0, 1, None, ynb), "x": (0, 2, None, xnb),
            "xa": (1, 3, A, xnb), "yb": (2, 3, B, ynb),
            "c0": (0, 4, None, cnb), "c1": (1, 5, None, cnb),
            "c2": (2, 6, None, cnb), "c3": (3, 7, None, cnb),
        }
        k = list(table).index(kind)
        sg, dg, cols, dev = table[kind]
        r = rows(zz)
        if cols is None:
            src, dst = X.at[sg, r], X.at[dg, r]
        else:
            src, dst = X.at[sg, r, cols], X.at[dg, r, cols]
        if own:
            src = x_in
        return rc(src, dst, ag_s.at[k, zz], ag_r.at[k, zz], dev)

    def each(fn, order):
        for s in order:
            if s == 0:
                fn(z, 0, 0)
            else:
                for side in (-1, 1):
                    zz = z + side * s
                    valid = (zz >= 0) & (zz < zn)

                    @pl.when(valid)
                    def _(zz=zz, s=s, side=side):
                        fn(zz, s, side)

    X[0, rows(z)] = x_in[...]

    def send_plane(zz):
        return rc(x_in, X.at[0, rows(z)], az_s.at[zz], az_r.at[z], plane(zz))

    def take_plane(zz):
        return rc(x_in, X.at[0, rows(zz)], az_s.at[zz], az_r.at[zz], plane(zz))

    def first(zz, s, side):
        own = s == 0
        if not own:
            take_plane(zz).wait_recv()
        for k in ("y", "x", "c0"):
            ag(k, zz, own).start()

    def second(zz, s, side):
        ag("y", zz).wait_recv()
        ag("xa", zz).start()
        ag("c1", zz).start()
        ag("x", zz).wait_recv()
        ag("yb", zz).start()
        ag("c2", zz).start()

    def third(zz, s, side):
        ag("xa", zz).wait_recv()
        ag("yb", zz).wait_recv()
        ag("c3", zz).start()

    def group_core(q):
        return rc(P1.at[q], crecv.at[q], c_s.at[q], c_r.at[q], cnb)

    def expert(g):
        xg = X[g, :, pl.ds(0, D)]
        gate = jnp.dot(xg, wg[...], preferred_element_type=jnp.float32)
        up = jnp.dot(xg, wu[...], preferred_element_type=jnp.float32)
        h = expert_act(gate, up).astype(jnp.bfloat16)
        tail = X[g, :, pl.ds(D, LANES)].astype(jnp.float32)
        lane = lax.broadcasted_iota(jnp.int32, tail.shape, 1)
        weight = jnp.sum(jnp.where(lane % (2 * zn) == sp, tail, 0.0), axis=1, keepdims=True)
        q = g % 4
        if g < 4:
            group_core(q).wait_recv()
        step = F
        for n in range(0, D, step):
            cols = pl.ds(n, step)
            part = jnp.dot(h, wd[:, cols], preferred_element_type=jnp.float32) * weight
            if g < 4:
                S[q, :, cols] = (part + crecv[q, :, cols].astype(jnp.float32)).astype(jnp.bfloat16)
            else:
                P1[q, :, cols] = part.astype(jnp.bfloat16)

    def core_arrivals(k):
        for zz in range(zn):
            ag(k, zz).wait_recv()

    lo, hi = pl.ds(0, H), pl.ds(H, H)

    def rs(kind, zz):
        r = rows(zz)
        table = {
            "yb": (S.at[1, r, hi], ry.at[r, hi], ynb),
            "xa": (S.at[2, r, lo], rx.at[r, lo], xnb),
            "dxa": (S.at[3, r, lo], rdx.at[r], xnb),
            "dyb": (S.at[3, r, hi], rdy.at[r], ynb),
            "ya": (S.at[1, r, lo], ry.at[r, lo], ynb),
            "xb": (S.at[2, r, hi], rx.at[r, hi], xnb),
        }
        k = list(table).index(kind)
        src, dst, dev = table[kind]
        return rc(src, dst, rs_s.at[k, zz], rs_r.at[k, zz], dev)

    def sum_plane(zz, source):
        return rc(S.at[0, rows(zz)], zbuf.at[rows(source)], rz_s.at[zz], rz_r.at[source], plane(zz))

    near = list(range(zn))
    each(lambda zz, s, side: send_plane(zz).start(), near[1:])

    for s in range(zn):
        each(first, [s])
        if s > 0:
            each(second, [s - 1])
    each(second, [zn - 1])
    for load in loads:
        load.wait()
    core_arrivals("c1")
    expert(5)
    group_core(1).start()
    expert(1)
    for zz in far_first:
        rs("yb", zz).start()
    core_arrivals("c2")
    expert(6)
    group_core(2).start()
    expert(2)
    for zz in far_first:
        rs("xa", zz).start()
    each(third, near)
    core_arrivals("c3")
    expert(7)
    group_core(3).start()
    expert(3)

    def diag(zz):
        rs("dxa", zz).start()
        rs("dyb", zz).start()

    for zz in far_first[:2]:
        diag(zz)
    core_arrivals("c0")
    expert(4)
    group_core(0).start()
    expert(0)

    f32 = jnp.float32

    def mid_sums(zz):
        r = rows(zz)
        rs("dxa", zz).wait_recv()
        S[1, r, lo] = (S[1, r, lo].astype(f32) + rdx[r].astype(f32)).astype(jnp.bfloat16)
        rs("ya", zz).start()
        rs("dyb", zz).wait_recv()
        S[2, r, hi] = (S[2, r, hi].astype(f32) + rdy[r].astype(f32)).astype(jnp.bfloat16)
        rs("xb", zz).start()

    def last_sums(zz):
        r = rows(zz)
        for k in ("xa", "xb", "ya", "yb"):
            rs(k, zz).wait_recv()
        return S[0, r].astype(f32) + rx[r].astype(f32) + ry[r].astype(f32)

    for k, zz in enumerate(far_first):
        mid_sums(zz)
        if k + 2 < zn:
            diag(far_first[k + 2])
        if k > 0:
            before = far_first[k - 1]
            S[0, rows(before)] = last_sums(before).astype(jnp.bfloat16)
            sum_plane(before, z).start()
    acc[...] = mid[...].astype(f32) + last_sums(z)
    for zz in far_first[:-1]:
        sum_plane(zz, zz).wait_recv()
        acc[...] += zbuf[rows(zz)].astype(f32)
    out[...] = acc[...].astype(jnp.bfloat16)

    def drain(zz, s, side):
        own = s == 0
        for k in ("y", "x", "c0"):
            ag(k, zz, own).wait_send()
        for k in ("xa", "yb", "c1", "c2", "c3"):
            ag(k, zz).wait_send()
        for k in ("yb", "xa", "dxa", "dyb", "ya", "xb"):
            rs(k, zz).wait_send()
        if not own:
            send_plane(zz).wait_send()
            sum_plane(zz, z).wait_send()

    each(drain, near)
    for q in range(4):
        group_core(q).wait_send()


def moe_exchange(x_in, middle, w_gate, w_up, w_down):
    zn = lax.axis_size("sp") // 2
    T, W = x_in.shape
    D = w_gate.shape[1]
    F = w_gate.shape[2]
    G = zn * T
    bf = jnp.bfloat16
    vm = pl.BlockSpec(memory_space=pltpu.VMEM)
    anyspec = pl.BlockSpec(memory_space=pl.ANY)
    return pl.pallas_call(
        functools.partial(moe_kernel, zn),
        out_shape=jax.ShapeDtypeStruct((T, D), bf),
        in_specs=[vm, vm, anyspec, anyspec, anyspec],
        out_specs=vm,
        scratch_shapes=[
            pltpu.VMEM((8, G, W), bf),
            pltpu.VMEM((4, G, D), bf),
            pltpu.VMEM((4, G, D), bf),
            pltpu.VMEM((4, G, D), bf),
            pltpu.VMEM((G, D), bf),
            pltpu.VMEM((G, D), bf),
            pltpu.VMEM((G, D // 2), bf),
            pltpu.VMEM((G, D // 2), bf),
            pltpu.VMEM((G, D), bf),
            pltpu.VMEM((T, D), jnp.float32),
            pltpu.VMEM((D, F), bf),
            pltpu.VMEM((D, F), bf),
            pltpu.VMEM((F, D), bf),
            pltpu.SemaphoreType.DMA((3,)),
            pltpu.SemaphoreType.DMA((zn,)),
            pltpu.SemaphoreType.DMA((zn,)),
            pltpu.SemaphoreType.DMA((8, zn)),
            pltpu.SemaphoreType.DMA((8, zn)),
            pltpu.SemaphoreType.DMA((4,)),
            pltpu.SemaphoreType.DMA((4,)),
            pltpu.SemaphoreType.DMA((6, zn)),
            pltpu.SemaphoreType.DMA((6, zn)),
            pltpu.SemaphoreType.DMA((zn,)),
            pltpu.SemaphoreType.DMA((zn,)),
        ],
        compiler_params=pltpu.CompilerParams(
            collective_id=1, has_side_effects=True, vmem_limit_bytes=VMEM_LIMIT
        ),
        name="moe_exchange",
    )(x_in, middle, w_gate, w_up, w_down)


def dense_fits(tokens, width, sp_size, tp_size, local_experts, hidden):
    experts = sp_size * local_experts
    gathered = tokens * (width + LANES) * 2
    buffers = gathered + tokens * width * 4 + 3 * hidden * width * 2
    return (
        tp_size == 4
        and sp_size % 2 == 0
        and local_experts == 1
        and 2 * experts <= LANES
        and width % (2 * LANES) == 0
        and width % hidden == 0
        and buffers < VMEM_LIMIT * 3 // 5
    )


def row_weights(own_routes, route_weights, expert_count):
    ids = jnp.arange(expert_count, dtype=jnp.int32)
    hit = own_routes[:, :, None] == ids[None, None, :]
    dense = jnp.sum(jnp.where(hit, route_weights[:, :, None], 0.0), axis=1)
    top = lax.reduce_precision(dense, 8, 7)
    low = dense - top
    both = jnp.concatenate([top, low], axis=1).astype(jnp.bfloat16)
    return jnp.pad(both, ((0, 0), (0, LANES - 2 * expert_count)))


def halo_kernel(peers, width, x, out, before, after, ss, rs):
    sp, tp = lax.axis_index("sp"), lax.axis_index("tp")
    length = x.shape[0]
    up, down = (sp + 1, tp), (sp - 1, tp)
    has_up, has_down = sp < peers - 1, sp > 0
    bar = pltpu.get_barrier_semaphore()

    def send(part, dst, i, dev):
        return pltpu.make_async_remote_copy(
            src_ref=part, dst_ref=dst, send_sem=ss.at[i], recv_sem=rs.at[i],
            device_id=dev, device_id_type=MESH,
        )

    go_up = send(x.at[pl.ds(length - width, width)], before, 0, up)
    go_down = send(x.at[pl.ds(0, width)], after, 1, down)

    @pl.when(has_up)
    def _():
        pl.semaphore_signal(bar, inc=1, device_id=up, device_id_type=MESH)

    @pl.when(has_down)
    def _():
        pl.semaphore_signal(bar, inc=1, device_id=down, device_id_type=MESH)

    pl.semaphore_wait(bar, has_up.astype(jnp.int32) + has_down.astype(jnp.int32))

    @pl.when(has_up)
    def _():
        go_up.start()

    @pl.when(has_down)
    def _():
        go_down.start()

    out[pl.ds(width, length)] = x[...]
    edge = jnp.zeros(before.shape, before.dtype)

    @pl.when(has_down)
    def _():
        go_up.wait_recv()
        out[pl.ds(0, width)] = before[...]

    @pl.when(jnp.logical_not(has_down))
    def _():
        out[pl.ds(0, width)] = edge

    @pl.when(has_up)
    def _():
        go_down.wait_recv()
        out[pl.ds(length + width, width)] = after[...]

    @pl.when(jnp.logical_not(has_up))
    def _():
        out[pl.ds(length + width, width)] = edge

    @pl.when(has_up)
    def _():
        go_up.wait_send()

    @pl.when(has_down)
    def _():
        go_down.wait_send()


def halo(x, width):
    length, columns = x.shape
    vm = pl.BlockSpec(memory_space=pltpu.VMEM)
    return pl.pallas_call(
        functools.partial(halo_kernel, lax.axis_size("sp"), width),
        out_shape=jax.ShapeDtypeStruct((length + 2 * width, columns), x.dtype),
        in_specs=[vm],
        out_specs=vm,
        scratch_shapes=[
            pltpu.VMEM((width, columns), x.dtype),
            pltpu.VMEM((width, columns), x.dtype),
            pltpu.SemaphoreType.DMA((2,)),
            pltpu.SemaphoreType.DMA((2,)),
        ],
        compiler_params=pltpu.CompilerParams(collective_id=2, has_side_effects=True),
        name="halo",
    )(x)


def swap_kernel(n, x, out, held, ss, rs):
    sp, me = lax.axis_index("sp"), lax.axis_index("tp")
    q, columns = out.shape[0], x.shape[1]
    bar = pltpu.get_barrier_semaphore()
    for p in range(1, n):
        pl.semaphore_signal(bar, inc=1, device_id=(sp, (me + p) % n), device_id_type=MESH)
    pl.semaphore_wait(bar, n - 1)

    def send(p):
        to = (me + p) % n
        part = pl.ds(pl.multiple_of(to * q, q), q)
        return pltpu.make_async_remote_copy(
            src_ref=x.at[part], dst_ref=held.at[me], send_sem=ss.at[p], recv_sem=rs.at[me],
            device_id=(sp, to), device_id_type=MESH,
        )

    for p in range(1, n):
        send(p).start()
    for s in range(n):
        cols = pl.ds(s * columns, columns)

        @pl.when(me == s)
        def _(cols=cols):
            out[:, cols] = x[pl.ds(pl.multiple_of(me * q, q), q)]

        @pl.when(me != s)
        def _(cols=cols, s=s):
            pltpu.make_async_remote_copy(
                src_ref=held.at[s], dst_ref=held.at[s], send_sem=ss.at[0], recv_sem=rs.at[s],
                device_id=(sp, (me + 1) % n), device_id_type=MESH,
            ).wait_recv()
            out[:, cols] = held[s]
    for p in range(1, n):
        send(p).wait_send()


def swap(x):
    n = lax.axis_size("tp")
    length, columns = x.shape
    vm = pl.BlockSpec(memory_space=pltpu.VMEM)
    return pl.pallas_call(
        functools.partial(swap_kernel, n),
        out_shape=jax.ShapeDtypeStruct((length // n, n * columns), x.dtype),
        in_specs=[vm],
        out_specs=vm,
        scratch_shapes=[
            pltpu.VMEM((n, length // n, columns), x.dtype),
            pltpu.SemaphoreType.DMA((n,)),
            pltpu.SemaphoreType.DMA((n,)),
        ],
        compiler_params=pltpu.CompilerParams(collective_id=3, has_side_effects=True),
        name="swap",
    )(x)


def per_device(
    resid,
    queries,
    keys,
    values,
    docs,
    q_gain,
    key_norm_gain,
    sink,
    out_gain,
    w_out,
    norm_gain,
    routes,
    route_weights,
    w_gate,
    w_up,
    w_down,
):
    sp_size = lax.axis_size("sp")
    tp_size = lax.axis_size("tp")
    sp_index = lax.axis_index("sp")
    tp_index = lax.axis_index("tp")
    tok_rows = queries.shape[0]
    head_size = q_gain.shape[0]
    query_heads = sink.shape[0]
    kv_heads = keys.shape[1] // head_size
    query_group_width = query_heads // kv_heads
    token_positions = (sp_index * tok_rows + jnp.arange(tok_rows, dtype=jnp.int32)).astype(
        jnp.float32
    )
    q_rot = apply_rotary_heads(
        row_normalize(queries.reshape(tok_rows, query_heads, head_size), q_gain), token_positions
    ).astype(jnp.bfloat16)
    key_rotated = apply_rotary_heads(
        row_normalize(keys.reshape(tok_rows, kv_heads, head_size), key_norm_gain), token_positions
    ).astype(jnp.bfloat16)
    key_value = jnp.concatenate(
        [key_rotated.reshape(tok_rows, kv_heads * head_size), values], axis=1
    )
    doc_mark = (docs + 1).astype(jnp.bfloat16)
    kv_width = key_value.shape[1]
    marks = jnp.broadcast_to(doc_mark[:, None], (tok_rows, LANES))
    packed_span = halo(jnp.concatenate([key_value, marks], axis=1), WINDOW)
    kv_span, doc_span = packed_span[:, :kv_width], packed_span[:, kv_width]
    span_rows = tok_rows + 2 * WINDOW
    k_span = kv_span[:, : kv_heads * head_size].reshape(span_rows, kv_heads, head_size)
    v_span = kv_span[:, kv_heads * head_size :].reshape(span_rows, kv_heads, head_size)
    scores = jnp.einsum(
        "qhgd,khd->hgqk",
        q_rot.reshape(tok_rows, kv_heads, query_group_width, head_size),
        k_span,
        preferred_element_type=jnp.float32,
    ) * head_size ** (-0.5)
    offsets = jnp.arange(tok_rows, dtype=jnp.int32)[:, None] - (
        jnp.arange(span_rows, dtype=jnp.int32)[None, :] - WINDOW
    )
    allowed = (jnp.abs(offsets) <= WINDOW) & (doc_mark[:, None] == doc_span[None, :])
    raw_weights = jnp.where(allowed[None, None], jnp.exp(scores), jnp.zeros((), jnp.float32))
    sink_exponent = jnp.exp(sink).reshape(kv_heads, query_group_width)
    total = jnp.sum(raw_weights, axis=-1) + sink_exponent[:, :, None]
    probs = (raw_weights / total[..., None]).astype(jnp.bfloat16)
    att = jnp.einsum("hgqk,khd->qhgd", probs, v_span, preferred_element_type=jnp.float32)
    att = att.astype(jnp.bfloat16).reshape(tok_rows, query_heads * head_size)
    by_token = swap(att)
    att_normed = row_normalize(by_token, out_gain).astype(jnp.bfloat16)
    middle = (
        resid.astype(jnp.float32) + jnp.dot(att_normed, w_out, preferred_element_type=jnp.float32)
    ).astype(jnp.bfloat16)
    moe_in = row_normalize(middle, norm_gain).astype(jnp.bfloat16)
    quarter = tok_rows // tp_size
    top_count = routes.shape[1]
    local_experts = w_gate.shape[0]
    expert_count = sp_size * local_experts
    capacity = 3 * quarter * top_count // (2 * expert_count) + 2
    model_width = moe_in.shape[1]
    empty = jnp.zeros((), jnp.bfloat16)
    own_routes = lax.dynamic_slice_in_dim(routes, tp_index * quarter, quarter, 0)
    if dense_fits(
        tok_rows * sp_size, model_width, sp_size, tp_size, local_experts, w_gate.shape[2]
    ):
        tail = row_weights(own_routes, route_weights, expert_count)
        packed = jnp.concatenate([moe_in, tail], axis=1)
        return moe_exchange(packed, middle, w_gate, w_up, w_down)
    pair_slot, slot_pair, filled = slot_tables(
        own_routes.reshape(1, quarter * top_count), expert_count, capacity
    )
    outgoing = jnp.where(filled[:, :, None], moe_in[slot_pair // top_count], empty)
    outgoing = outgoing.reshape(1, sp_size, local_experts * capacity, model_width)
    arrived = lax.all_to_all(outgoing, "sp", split_axis=1, concat_axis=1, tiled=True)
    terms = expert_partial(lax.all_gather(arrived, "tp", axis=0, tiled=True), w_gate, w_up, w_down)
    summed = lax.psum_scatter(terms.astype(jnp.bfloat16), "tp", scatter_dimension=0, tiled=True)
    own_slot = pair_slot[0]
    returned = lax.all_to_all(summed, "sp", split_axis=1, concat_axis=1, tiled=True)
    picked = returned.reshape(-1, model_width)[own_slot].reshape(quarter, top_count, model_width)
    routed = jnp.sum(picked.astype(jnp.float32) * route_weights[:, :, None], axis=1)
    return (middle.astype(jnp.float32) + routed).astype(jnp.bfloat16)


def solution(mesh):
    return jax.shard_map(
        per_device,
        mesh=mesh,
        in_specs=(
            P(("sp", "tp"), None),
            P("sp", "tp"),
            P("sp", "tp"),
            P("sp", "tp"),
            P("sp"),
            P(),
            P(),
            P("tp"),
            P(),
            P(),
            P(),
            P("sp", None),
            P(("sp", "tp"), None),
            P("sp", None, "tp"),
            P("sp", None, "tp"),
            P("sp", "tp", None),
        ),
        out_specs=P(("sp", "tp"), None),
        check_vma=False,
    )
```

```python
import functools

import jax
import jax.numpy as jnp
from jax import lax
from jax.experimental import pallas as pl
from jax.experimental.pallas import tpu as pltpu
from jax.sharding import PartitionSpec as P

rope_base = 10000.0
norm_eps = 1e-06
swiglu_limit = 7.0
swiglu_alpha = 1.702


def expert_act(gate_pre, up_pre):
    gate_cut = jnp.minimum(gate_pre, swiglu_limit)
    up_cut = jnp.clip(up_pre, -swiglu_limit, swiglu_limit)
    return (up_cut + 1.0) * gate_cut * jax.nn.sigmoid(swiglu_alpha * gate_cut)


def slot_tables(route_block, expert_count, capacity):
    pair_total = route_block.shape[1]
    expert_ids = jnp.arange(expert_count, dtype=jnp.int32)
    onehot = (route_block[:, :, None] == expert_ids[None, None, :]).astype(jnp.int32)
    before = jnp.cumsum(onehot, axis=1) - onehot
    rank = jnp.sum(before * onehot, axis=-1)
    pair_slot = route_block * capacity + rank
    slot_ids = jnp.arange(expert_count * capacity, dtype=jnp.int32)
    match = pair_slot[:, :, None] == slot_ids[None, None, :]
    pair_ids = jnp.arange(pair_total, dtype=jnp.int32)
    slot_pair = jnp.sum(jnp.where(match, pair_ids[None, :, None], 0), axis=1)
    filled = jnp.any(match, axis=1)
    return (pair_slot, slot_pair, filled)


def expert_partial(arrived_rows, w_gate, w_up, w_down):
    lead_shape = arrived_rows.shape
    local_experts = w_gate.shape[0]
    grouped = arrived_rows.reshape(-1, local_experts, lead_shape[2] // local_experts, lead_shape[3])
    gate_pre = jnp.einsum("recd,edf->recf", grouped, w_gate, preferred_element_type=jnp.float32)
    up_pre = jnp.einsum("recd,edf->recf", grouped, w_up, preferred_element_type=jnp.float32)
    hidden = expert_act(gate_pre, up_pre).astype(jnp.bfloat16)
    partial_value = jnp.einsum("recf,efd->recd", hidden, w_down, preferred_element_type=jnp.float32)
    return (
        lax.optimization_barrier(partial_value.astype(jnp.bfloat16))
        .astype(jnp.float32)
        .reshape(lead_shape)
    )


LANES = 128
VMEM_LIMIT = 60 * 1024 * 1024
MESH = pl.DeviceIdType.MESH


def moe_kernel(
    zn, x_in, mid, wg_hbm, wu_hbm, wd_hbm, out,
    X, S, P1, crecv, rx, ry, rdx, rdy, zbuf, acc, wg, wu, wd,
    wsem, ag_s, ag_r, c_s, c_r, rs_s, rs_r, rz_s, rz_r,
):
    sp, tp = lax.axis_index("sp"), lax.axis_index("tp")
    z, y = sp // 2, sp % 2
    xx, c = tp // 2, tp % 2
    T, W = x_in.shape
    D = out.shape[1]
    H = D // 2
    F = wg.shape[1]
    ynb = (z * 2 + (1 - y), tp)
    xnb = (sp, (1 - xx) * 2 + c)
    cnb = (sp, xx * 2 + (1 - c))

    def plane(zz):
        return (zz * 2 + y, tp)

    right, left = plane(z + 1), plane(z - 1)
    has_r, has_l = z < zn - 1, z > 0

    turn = 2 * (2 * z // zn) - 1
    far_first = [(z + turn * (1 + k) + 2 * zn) % zn for k in range(zn - 1)] + [z]

    loads = [
        pltpu.make_async_copy(src.at[0], dst, wsem.at[i])
        for i, (src, dst) in enumerate(((wg_hbm, wg), (wu_hbm, wu), (wd_hbm, wd)))
    ]
    for load in loads:
        load.start()

    bar = pltpu.get_barrier_semaphore()
    for nb in (ynb, xnb, cnb, *(plane(zz) for zz in far_first[:-1])):
        pl.semaphore_signal(bar, inc=1, device_id=nb, device_id_type=MESH)
    pl.semaphore_wait(bar, 3 + zn - 1)

    def rows(zz):
        return pl.ds(pl.multiple_of(zz * T, T), T)

    def rc(src, dst, ss, rs, dev):
        return pltpu.make_async_remote_copy(
            src_ref=src, dst_ref=dst, send_sem=ss, recv_sem=rs, device_id=dev, device_id_type=MESH
        )

    A, B = pl.ds(0, H), pl.ds(H, W - H)

    def ag(kind, zz, own=False):
        table = {
            "zr": (0, 0, None, right), "zl": (0, 0, None, left),
            "y": (0, 1, None, ynb), "x": (0, 2, None, xnb),
            "xa": (1, 3, A, xnb), "yb": (2, 3, B, ynb),
            "c0": (0, 4, None, cnb), "c1": (1, 5, None, cnb),
            "c2": (2, 6, None, cnb), "c3": (3, 7, None, cnb),
        }
        k = list(table).index(kind)
        sg, dg, cols, dev = table[kind]
        r = rows(zz)
        if cols is None:
            src, dst = X.at[sg, r], X.at[dg, r]
        else:
            src, dst = X.at[sg, r, cols], X.at[dg, r, cols]
        if own:
            src = x_in
        return rc(src, dst, ag_s.at[k, zz], ag_r.at[k, zz], dev)

    def each(fn, order):
        for s in order:
            if s == 0:
                fn(z, 0, 0)
            else:
                for side in (-1, 1):
                    zz = z + side * s
                    valid = (zz >= 0) & (zz < zn)

                    @pl.when(valid)
                    def _(zz=zz, s=s, side=side):
                        fn(zz, s, side)

    X[0, rows(z)] = x_in[...]

    def first(zz, s, side):
        own = s == 0
        if side == -1:
            ag("zr", zz).wait_recv()
        if side == 1:
            ag("zl", zz).wait_recv()
        if side <= 0:
            @pl.when(has_r)
            def _():
                ag("zr", zz, own).start()
        if side >= 0:
            @pl.when(has_l)
            def _():
                ag("zl", zz, own).start()
        for k in ("y", "x", "c0"):
            ag(k, zz, own).start()

    def second(zz, s, side):
        ag("y", zz).wait_recv()
        ag("xa", zz).start()
        ag("c1", zz).start()
        ag("x", zz).wait_recv()
        ag("yb", zz).start()
        ag("c2", zz).start()

    def third(zz, s, side):
        ag("xa", zz).wait_recv()
        ag("yb", zz).wait_recv()
        ag("c3", zz).start()

    def group_core(q):
        return rc(P1.at[q], crecv.at[q], c_s.at[q], c_r.at[q], cnb)

    def expert(g):
        xg = X[g, :, pl.ds(0, D)]
        gate = jnp.dot(xg, wg[...], preferred_element_type=jnp.float32)
        up = jnp.dot(xg, wu[...], preferred_element_type=jnp.float32)
        h = expert_act(gate, up).astype(jnp.bfloat16)
        tail = X[g, :, pl.ds(D, LANES)].astype(jnp.float32)
        lane = lax.broadcasted_iota(jnp.int32, tail.shape, 1)
        weight = jnp.sum(jnp.where(lane % (2 * zn) == sp, tail, 0.0), axis=1, keepdims=True)
        q = g % 4
        if g < 4:
            group_core(q).wait_recv()
        step = F
        for n in range(0, D, step):
            cols = pl.ds(n, step)
            part = jnp.dot(h, wd[:, cols], preferred_element_type=jnp.float32) * weight
            if g < 4:
                S[q, :, cols] = (part + crecv[q, :, cols].astype(jnp.float32)).astype(jnp.bfloat16)
            else:
                P1[q, :, cols] = part.astype(jnp.bfloat16)

    def core_arrivals(k):
        for zz in range(zn):
            ag(k, zz).wait_recv()

    lo, hi = pl.ds(0, H), pl.ds(H, H)

    def rs(kind, zz):
        r = rows(zz)
        table = {
            "yb": (S.at[1, r, hi], ry.at[r, hi], ynb),
            "xa": (S.at[2, r, lo], rx.at[r, lo], xnb),
            "dxa": (S.at[3, r, lo], rdx.at[r], xnb),
            "dyb": (S.at[3, r, hi], rdy.at[r], ynb),
            "ya": (S.at[1, r, lo], ry.at[r, lo], ynb),
            "xb": (S.at[2, r, hi], rx.at[r, hi], xnb),
        }
        k = list(table).index(kind)
        src, dst, dev = table[kind]
        return rc(src, dst, rs_s.at[k, zz], rs_r.at[k, zz], dev)

    def sum_plane(zz, source):
        return rc(S.at[0, rows(zz)], zbuf.at[rows(source)], rz_s.at[zz], rz_r.at[source], plane(zz))

    near = list(range(zn))

    for s in range(zn):
        each(first, [s])
        if s > 0:
            each(second, [s - 1])
    each(second, [zn - 1])
    for load in loads:
        load.wait()
    core_arrivals("c1")
    expert(5)
    group_core(1).start()
    expert(1)
    for zz in far_first:
        rs("yb", zz).start()
    core_arrivals("c2")
    expert(6)
    group_core(2).start()
    expert(2)
    for zz in far_first:
        rs("xa", zz).start()
    each(third, near)
    core_arrivals("c3")
    expert(7)
    group_core(3).start()
    expert(3)

    def diag(zz):
        rs("dxa", zz).start()
        rs("dyb", zz).start()

    for zz in far_first[:2]:
        diag(zz)
    core_arrivals("c0")
    expert(4)
    group_core(0).start()
    expert(0)

    f32 = jnp.float32

    def mid_sums(zz):
        r = rows(zz)
        rs("dxa", zz).wait_recv()
        S[1, r, lo] = (S[1, r, lo].astype(f32) + rdx[r].astype(f32)).astype(jnp.bfloat16)
        rs("ya", zz).start()
        rs("dyb", zz).wait_recv()
        S[2, r, hi] = (S[2, r, hi].astype(f32) + rdy[r].astype(f32)).astype(jnp.bfloat16)
        rs("xb", zz).start()

    def last_sums(zz):
        r = rows(zz)
        for k in ("xa", "xb", "ya", "yb"):
            rs(k, zz).wait_recv()
        return S[0, r].astype(f32) + rx[r].astype(f32) + ry[r].astype(f32)

    for k, zz in enumerate(far_first):
        mid_sums(zz)
        if k + 2 < zn:
            diag(far_first[k + 2])
        if k > 0:
            before = far_first[k - 1]
            S[0, rows(before)] = last_sums(before).astype(jnp.bfloat16)
            sum_plane(before, z).start()
    acc[...] = mid[...].astype(f32) + last_sums(z)
    for zz in far_first[:-1]:
        sum_plane(zz, zz).wait_recv()
        acc[...] += zbuf[rows(zz)].astype(f32)
    out[...] = acc[...].astype(jnp.bfloat16)

    def drain(zz, s, side):
        own = s == 0
        if side <= 0:
            @pl.when(has_r)
            def _():
                ag("zr", zz, own).wait_send()
        if side >= 0:
            @pl.when(has_l)
            def _():
                ag("zl", zz, own).wait_send()
        for k in ("y", "x", "c0"):
            ag(k, zz, own).wait_send()
        for k in ("xa", "yb", "c1", "c2", "c3"):
            ag(k, zz).wait_send()
        for k in ("yb", "xa", "dxa", "dyb", "ya", "xb"):
            rs(k, zz).wait_send()
        if not own:
            sum_plane(zz, z).wait_send()

    each(drain, near)
    for q in range(4):
        group_core(q).wait_send()


def moe_exchange(x_in, middle, w_gate, w_up, w_down):
    zn = lax.axis_size("sp") // 2
    T, W = x_in.shape
    D = w_gate.shape[1]
    F = w_gate.shape[2]
    G = zn * T
    bf = jnp.bfloat16
    vm = pl.BlockSpec(memory_space=pltpu.VMEM)
    anyspec = pl.BlockSpec(memory_space=pl.ANY)
    return pl.pallas_call(
        functools.partial(moe_kernel, zn),
        out_shape=jax.ShapeDtypeStruct((T, D), bf),
        in_specs=[vm, vm, anyspec, anyspec, anyspec],
        out_specs=vm,
        scratch_shapes=[
            pltpu.VMEM((8, G, W), bf),
            pltpu.VMEM((4, G, D), bf),
            pltpu.VMEM((4, G, D), bf),
            pltpu.VMEM((4, G, D), bf),
            pltpu.VMEM((G, D), bf),
            pltpu.VMEM((G, D), bf),
            pltpu.VMEM((G, D // 2), bf),
            pltpu.VMEM((G, D // 2), bf),
            pltpu.VMEM((G, D), bf),
            pltpu.VMEM((T, D), jnp.float32),
            pltpu.VMEM((D, F), bf),
            pltpu.VMEM((D, F), bf),
            pltpu.VMEM((F, D), bf),
            pltpu.SemaphoreType.DMA((3,)),
            pltpu.SemaphoreType.DMA((10, zn)),
            pltpu.SemaphoreType.DMA((10, zn)),
            pltpu.SemaphoreType.DMA((4,)),
            pltpu.SemaphoreType.DMA((4,)),
            pltpu.SemaphoreType.DMA((6, zn)),
            pltpu.SemaphoreType.DMA((6, zn)),
            pltpu.SemaphoreType.DMA((zn,)),
            pltpu.SemaphoreType.DMA((zn,)),
        ],
        compiler_params=pltpu.CompilerParams(
            collective_id=1, has_side_effects=True, vmem_limit_bytes=VMEM_LIMIT
        ),
        name="moe_exchange",
    )(x_in, middle, w_gate, w_up, w_down)


def dense_fits(tokens, width, sp_size, tp_size, local_experts, hidden):
    experts = sp_size * local_experts
    gathered = tokens * (width + LANES) * 2
    buffers = gathered + tokens * width * 4 + 3 * hidden * width * 2
    return (
        tp_size == 4
        and sp_size % 2 == 0
        and local_experts == 1
        and 2 * experts <= LANES
        and width % (2 * LANES) == 0
        and width % hidden == 0
        and buffers < VMEM_LIMIT * 3 // 5
    )


def row_weights(own_routes, route_weights, expert_count):
    ids = jnp.arange(expert_count, dtype=jnp.int32)
    hit = own_routes[:, :, None] == ids[None, None, :]
    dense = jnp.sum(jnp.where(hit, route_weights[:, :, None], 0.0), axis=1)
    top = lax.reduce_precision(dense, 8, 7)
    low = dense - top
    both = jnp.concatenate([top, low], axis=1).astype(jnp.bfloat16)
    return jnp.pad(both, ((0, 0), (0, LANES - 2 * expert_count)))


def front_kernel(
    peers, n, q_in, k_in, v_in, docs_row, angle_in, q_gain, k_gain, sink,
    out_gain, resid, norm_gain, tail, w_hbm, mid, packed,
    kv, span, att, held, w, wsem, kv_s, kv_r, doc_s, doc_r, ss, rs,
):
    sp, me = lax.axis_index("sp"), lax.axis_index("tp")
    f32, bf = jnp.float32, jnp.bfloat16
    head, length = k_in.shape
    width = LANES
    half = head // 2
    heads = q_in.shape[1] // head
    blocks = length // width
    part_rows = length // n
    D = mid.shape[1]
    up, down = (sp + 1, me), (sp - 1, me)
    has_up, has_down = sp < peers - 1, sp > 0
    load = pltpu.make_async_copy(w_hbm, w, wsem.at[0])
    load.start()

    bar = pltpu.get_barrier_semaphore()
    for p in range(1, n):
        pl.semaphore_signal(bar, inc=1, device_id=(sp, (me + p) % n), device_id_type=MESH)

    @pl.when(has_up)
    def _():
        pl.semaphore_signal(bar, inc=1, device_id=up, device_id_type=MESH)

    @pl.when(has_down)
    def _():
        pl.semaphore_signal(bar, inc=1, device_id=down, device_id_type=MESH)

    def rc(src, dst, send_sem, recv_sem, dev):
        return pltpu.make_async_remote_copy(
            src_ref=src, dst_ref=dst, send_sem=send_sem, recv_sem=recv_sem,
            device_id=dev, device_id_type=MESH,
        )

    go_up = (
        rc(kv.at[pl.ds(length, width)], kv.at[pl.ds(0, width)], kv_s.at[0], kv_r.at[0], up),
        rc(docs_row.at[blocks - 1], span.at[0], doc_s.at[0], doc_r.at[0], up),
    )
    go_down = (
        rc(kv.at[pl.ds(width, width)], kv.at[pl.ds(length + width, width)], kv_s.at[1], kv_r.at[1], down),
        rc(docs_row.at[0], span.at[blocks + 1], doc_s.at[1], doc_r.at[1], down),
    )
    table = jnp.transpose(jnp.concatenate([angle_in[...]] * 2, axis=0))
    cosine, sine = table[:, :half], table[:, half:head]
    own = jnp.concatenate([k_in[...].astype(f32), v_in[...].astype(f32)], axis=0)
    own = jnp.transpose(own)

    def rotated(x, gain):
        x = x * lax.rsqrt(jnp.mean(x * x, axis=1, keepdims=True) + norm_eps) * gain
        a, b = x[:, :half], x[:, half:]
        return jnp.concatenate([a * cosine - b * sine, a * sine + b * cosine], axis=1).astype(bf)

    kv[pl.ds(width, length)] = jnp.concatenate(
        [rotated(own[:, :head], k_gain[...]), own[:, head:].astype(bf)], axis=1
    )
    pl.semaphore_wait(bar, n - 1 + has_up.astype(jnp.int32) + has_down.astype(jnp.int32))

    @pl.when(has_up)
    def _():
        for copy in go_up:
            copy.start()

    @pl.when(has_down)
    def _():
        for copy in go_down:
            copy.start()

    span[pl.ds(1, blocks)] = docs_row[...]

    @pl.when(jnp.logical_not(has_down))
    def _():
        kv[pl.ds(0, width)] = jnp.zeros((width, 2 * head), bf)
        span[0] = jnp.full((1, width), -1, jnp.int32)

    @pl.when(jnp.logical_not(has_up))
    def _():
        kv[pl.ds(length + width, width)] = jnp.zeros((width, 2 * head), bf)
        span[blocks + 1] = jnp.full((1, width), -1, jnp.int32)

    queries = q_in[...].astype(f32)
    q_rot = [rotated(queries[:, h * head : (h + 1) * head], q_gain[...]) for h in range(heads)]

    @pl.when(has_down)
    def _():
        for copy in go_up:
            copy.wait_recv()

    @pl.when(has_up)
    def _():
        for copy in go_down:
            copy.wait_recv()

    row = lax.broadcasted_iota(jnp.int32, (width, width), 0)
    col = lax.broadcasted_iota(jnp.int32, (width, width), 1)
    for b in range(blocks):
        own_doc = jnp.broadcast_to(docs_row[b].astype(f32), (width, width))
        own_doc = jnp.transpose(own_doc)
        same = [own_doc == span[b + j].astype(f32) for j in range(3)]
        allowed = jnp.concatenate([same[0] & (col >= row), same[1], same[2] & (col <= row)], axis=1)
        both = kv[pl.ds(b * width, 3 * width)]
        key_rows, value_rows = both[:, :head], both[:, head:]
        mixed = []
        for h in range(heads):
            scores = lax.dot_general(
                q_rot[h][b * width : (b + 1) * width], key_rows, (((1,), (1,)), ((), ())),
                preferred_element_type=f32,
            )
            raw = jnp.where(allowed, jnp.exp(scores * head**-0.5), 0.0)
            total = jnp.sum(raw, axis=1, keepdims=True) + jnp.exp(jnp.full((1, 1), sink[h]))
            probs = (raw / total).astype(bf)
            mixed.append(jnp.dot(probs, value_rows, preferred_element_type=f32))
        att[pl.ds(b * width, width)] = jnp.concatenate(mixed, axis=1).astype(bf)

    def own_part(to):
        return pl.ds(pl.multiple_of(to * part_rows, part_rows), part_rows)

    def swap(p):
        to = (me + p) % n
        return rc(att.at[own_part(to)], held.at[me], ss.at[p], rs.at[me], (sp, to))

    def arrival(p):
        source = (me + p) % n
        return rc(held.at[source], held.at[source], ss.at[0], rs.at[source], (sp, source))

    for p in range(1, n):
        swap(p).start()
    held[me] = att[own_part(me)]
    for p in range(1, n):
        arrival(p).wait_recv()
    by_token = jnp.concatenate([held[s] for s in range(n)], axis=1).astype(f32)
    inverse = lax.rsqrt(jnp.mean(by_token * by_token, axis=1, keepdims=True) + norm_eps)
    att_normed = (by_token * inverse * out_gain[...]).astype(bf)
    load.wait()
    step = D // 4
    squares = jnp.zeros((part_rows, 1), f32)
    for c in range(0, D, step):
        cols = pl.ds(c, step)
        value = jnp.dot(att_normed, w[:, cols], preferred_element_type=f32)
        value = (resid[:, cols].astype(f32) + value).astype(bf)
        mid[:, cols] = value
        value = value.astype(f32)
        squares = squares + jnp.sum(value * value, axis=1, keepdims=True)
    inverse = lax.rsqrt(squares / D + norm_eps)
    for c in range(0, D, step):
        cols = pl.ds(c, step)
        packed[:, cols] = (mid[:, cols].astype(f32) * inverse * norm_gain[:, cols]).astype(bf)
    packed[:, pl.ds(D, LANES)] = tail[...]

    @pl.when(has_up)
    def _():
        for copy in go_up:
            copy.wait_send()

    @pl.when(has_down)
    def _():
        for copy in go_down:
            copy.wait_send()

    for p in range(1, n):
        swap(p).wait_send()


def front(
    queries, keys, values, docs, angle_table, q_gain, key_norm_gain, sink,
    out_gain, resid, norm_gain, tail, w_out,
):
    n = lax.axis_size("tp")
    length, head = keys.shape
    columns = queries.shape[1]
    rows, D = resid.shape
    bf = jnp.bfloat16
    blocks = length // LANES
    vm = pl.BlockSpec(memory_space=pltpu.VMEM)
    smem = pl.BlockSpec(memory_space=pltpu.SMEM)
    return pl.pallas_call(
        functools.partial(front_kernel, lax.axis_size("sp"), n),
        out_shape=(
            jax.ShapeDtypeStruct((rows, D), bf),
            jax.ShapeDtypeStruct((rows, D + LANES), bf),
        ),
        in_specs=[vm] * 7 + [smem] + [vm] * 4 + [pl.BlockSpec(memory_space=pl.ANY)],
        out_specs=(vm, vm),
        scratch_shapes=[
            pltpu.VMEM((length + 2 * LANES, 2 * head), bf),
            pltpu.VMEM((blocks + 2, 1, LANES), jnp.int32),
            pltpu.VMEM((length, columns), bf),
            pltpu.VMEM((n, rows, columns), bf),
            pltpu.VMEM(w_out.shape, bf),
            pltpu.SemaphoreType.DMA((1,)),
            pltpu.SemaphoreType.DMA((2,)),
            pltpu.SemaphoreType.DMA((2,)),
            pltpu.SemaphoreType.DMA((2,)),
            pltpu.SemaphoreType.DMA((2,)),
            pltpu.SemaphoreType.DMA((n,)),
            pltpu.SemaphoreType.DMA((n,)),
        ],
        compiler_params=pltpu.CompilerParams(
            collective_id=2, has_side_effects=True, vmem_limit_bytes=VMEM_LIMIT
        ),
        name="front",
    )(
        queries, keys.T, values.T, docs.reshape(blocks, 1, LANES), angle_table,
        q_gain[None], key_norm_gain[None], sink, out_gain[None], resid, norm_gain[None], tail, w_out,
    )


def per_device(
    resid,
    queries,
    keys,
    values,
    docs,
    q_gain,
    key_norm_gain,
    sink,
    out_gain,
    w_out,
    norm_gain,
    routes,
    route_weights,
    w_gate,
    w_up,
    w_down,
):
    sp_size = lax.axis_size("sp")
    tp_size = lax.axis_size("tp")
    sp_index = lax.axis_index("sp")
    tp_index = lax.axis_index("tp")
    tok_rows = queries.shape[0]
    half_size = q_gain.shape[0] // 2
    token_positions = (sp_index * tok_rows + jnp.arange(tok_rows, dtype=jnp.int32)).astype(
        jnp.float32
    )
    freqs = rope_base ** (-jnp.arange(half_size, dtype=jnp.float32) / half_size)
    angles = freqs[:, None] * token_positions[None, :]
    angle_table = jnp.concatenate([jnp.cos(angles), jnp.sin(angles)], axis=0)
    quarter = tok_rows // tp_size
    top_count = routes.shape[1]
    local_experts = w_gate.shape[0]
    expert_count = sp_size * local_experts
    capacity = 3 * quarter * top_count // (2 * expert_count) + 2
    model_width = resid.shape[1]
    empty = jnp.zeros((), jnp.bfloat16)
    own_routes = lax.dynamic_slice_in_dim(routes, tp_index * quarter, quarter, 0)
    dense = dense_fits(
        tok_rows * sp_size, model_width, sp_size, tp_size, local_experts, w_gate.shape[2]
    )
    if dense:
        tail = row_weights(own_routes, route_weights, expert_count)
    else:
        tail = jnp.zeros((quarter, LANES), jnp.bfloat16)
    middle, packed = front(
        queries, keys, values, docs, angle_table, q_gain, key_norm_gain, sink,
        out_gain, resid, norm_gain, tail, w_out,
    )
    if dense:
        return moe_exchange(packed, middle, w_gate, w_up, w_down)
    moe_in = packed[:, :model_width]
    pair_slot, slot_pair, filled = slot_tables(
        own_routes.reshape(1, quarter * top_count), expert_count, capacity
    )
    outgoing = jnp.where(filled[:, :, None], moe_in[slot_pair // top_count], empty)
    outgoing = outgoing.reshape(1, sp_size, local_experts * capacity, model_width)
    arrived = lax.all_to_all(outgoing, "sp", split_axis=1, concat_axis=1, tiled=True)
    terms = expert_partial(lax.all_gather(arrived, "tp", axis=0, tiled=True), w_gate, w_up, w_down)
    summed = lax.psum_scatter(terms.astype(jnp.bfloat16), "tp", scatter_dimension=0, tiled=True)
    own_slot = pair_slot[0]
    returned = lax.all_to_all(summed, "sp", split_axis=1, concat_axis=1, tiled=True)
    picked = returned.reshape(-1, model_width)[own_slot].reshape(quarter, top_count, model_width)
    routed = jnp.sum(picked.astype(jnp.float32) * route_weights[:, :, None], axis=1)
    return (middle.astype(jnp.float32) + routed).astype(jnp.bfloat16)


def solution(mesh):
    return jax.shard_map(
        per_device,
        mesh=mesh,
        in_specs=(
            P(("sp", "tp"), None),
            P("sp", "tp"),
            P("sp", "tp"),
            P("sp", "tp"),
            P("sp"),
            P(),
            P(),
            P("tp"),
            P(),
            P(),
            P(),
            P("sp", None),
            P(("sp", "tp"), None),
            P("sp", None, "tp"),
            P("sp", None, "tp"),
            P("sp", "tp", None),
        ),
        out_specs=P(("sp", "tp"), None),
        check_vma=False,
    )
```
